256 devices in a mesh: grp: 2 (over y), st: 32 (over z, core), tp: 4 (over x).
Axes of the slice: x: 4, y: 2, z: 16, core: 2. Of those that a mesh axis runs over, the one named last changes fastest.
The devices are a block of a 4x16x16 slice.
Arguments:
- tokens: bfloat16 [65536, 2048], P(('grp', 'st'), 'tp'), parts along dimension 0, may hold values from -6 to 6
- norm_gain: float32 [2048], replicated, may hold values from 0.1 to 1.9
- pool_weight: bfloat16 [4, 512, 512], P('tp'), may hold values from -0.25 to 0.25
- pool_scale: float32 [2048], P('tp'), may hold values from 0.1 to 1.9
- query_weight: bfloat16 [2048, 1024], P(None, 'tp'), may hold values from -3 to 3
- gate_weight: bfloat16 [2048, 8], replicated, may hold values from -0.125 to 0.125
- key_weight: bfloat16 [2048, 1024], P(None, 'tp'), may hold values from -0.125 to 0.125
- value_weight: bfloat16 [2048, 1024], P(None, 'tp'), may hold values from -0.125 to 0.125
- out_weight: bfloat16 [1024, 2048], P(None, 'tp'), may hold values from -0.1875 to 0.1875
- passage_gain: float32 [2048], replicated, may hold values from 0.1 to 1.9
- passage_store: bfloat16 [1536, 64, 2048], P(('grp', 'st')), parts along dimension 0, may hold values from -6 to 6
- passage_ids: int32 [512, 4], P(('grp', 'st')), parts along dimension 0, may hold values from 0 to 767, as said below
Outputs:
- mixed: bfloat16 [65536, 2048], P(('grp', 'st'), 'tp'), parts along dimension 0
The draws below stay inside these ranges and needn't reach their ends.
There are 2 independent parts, one for each index of `grp`. The reference program is written for one: setup_inputs(seed, part) draws one part's arguments, and reference() takes and returns one part's arrays. A program takes and returns all parts, laid end to end along the dimension named above; an argument that names none is the same for every part. Nothing has to cross between parts.
Inputs may be any that keep to these rules, and one draw needn't show every extreme that they name: `passage_ids`: the ids of the blocks of one index of st name at most 2 passages held by any one index of st, and exactly 2 held by some index.
All inputs are finite; a program needn't handle non-finite values.
Results may differ from the reference program's by a relative error of at most 0.009.
Values may be sent and summed in bfloat16 or wider, within the bound.
A program may use at most 128 MiB of HBM per device.

```python
import jax
import jax.numpy as jnp
from jax import lax

D = 2048
HEADS = 8
HD = 128
GROUPS = 4
GROUP_CH = 512
SEQ_LEN = 256
BLK = 128
NPB = 4
PLEN = 64
P_DEV = 24
TOKENS = 32768
BLK_DEV = 8
BLOCKS = 256
REQ = 32
CAP = 2
PASSAGES = 768
N_ST = 32


def draw_passage_ids(key, part):
    base_key = jax.random.fold_in(key, 11)
    slots_all = N_ST * CAP
    tickets = jnp.arange(slots_all, dtype=jnp.int32)
    ticket_owner = tickets // CAP

    def one_reader(reader_key, reader):
        order_key, full_key, shuffle_key, first_key, second_key = jax.random.split(reader_key, 5)
        base_rank = jax.random.permutation(order_key, slots_all).astype(jnp.int32)
        full_owner = jax.random.randint(full_key, (), 0, N_ST, dtype=jnp.int32)
        before = (reader + N_ST - 1) % N_ST
        halfway = (reader + N_ST // 2) % N_ST
        forced = (tickets == before * CAP) | (tickets == halfway * CAP)
        ranking = base_rank - 3 * slots_all * (ticket_owner == full_owner).astype(jnp.int32) - slots_all * forced.astype(jnp.int32)
        chosen = jnp.argsort(ranking, stable=True)[:REQ]
        owners = ticket_owner[chosen]
        owners = owners[jax.random.permutation(shuffle_key, REQ)]
        local_index = jnp.minimum(jax.random.randint(first_key, (REQ,), 0, P_DEV, dtype=jnp.int32), jax.random.randint(second_key, (REQ,), 0, P_DEV, dtype=jnp.int32))
        return (owners * P_DEV + local_index).reshape(BLK_DEV, NPB)
    reader_keys = jax.random.split(base_key, N_ST)
    readers = jnp.arange(N_ST, dtype=jnp.int32)
    return jax.vmap(one_reader)(reader_keys, readers).reshape(BLOCKS, NPB).astype(jnp.int32)


def draw_query_weight(key, part):
    base_key = jax.random.fold_in(key, 23)
    normal_key = jax.random.fold_in(base_key, 0)
    weights = jax.random.normal(normal_key, (D, HEADS * HD), jnp.float32) * D ** (-0.5)
    return jnp.clip(weights, -3.0, 3.0).astype(jnp.bfloat16)


def shard_levels(stream_key, shape, shards, least, largest):
    level = 1.0
    for dim, parts in shards:
        draws = jax.random.uniform(jax.random.fold_in(jax.random.fold_in(stream_key, 6), dim), (parts,), jnp.float32, least / len(shards), largest / len(shards))
        level = level * jnp.repeat(jnp.exp(draws), shape[dim] // parts).reshape((-1,) + (1,) * (len(shape) - 1 - dim))
    return level


def gaussian(own_key, shape, spread, bound, cuts=(), kind=jnp.bfloat16):
    factor_of = shard_levels(own_key, shape, cuts, -0.22, 0.18) if cuts else 1.0
    values = jax.random.normal(own_key, shape, jnp.float32) * spread * factor_of
    return jnp.minimum(jnp.maximum(values, -bound), bound).astype(kind)


def setup_inputs(seed: int = 0, part: int = 0) -> dict:
    arg_keys = jax.random.split(jax.random.key(seed), 13)
    part_splits = jax.random.split(jax.random.fold_in(arg_keys[12], part), 13)
    tokens = gaussian(part_splits[0], (TOKENS, D), 1.0, 6.0, ((0, 32), (1, 4)))
    norm_gain = jnp.clip(1.0 + 0.18 * jax.random.normal(arg_keys[1], (D,), jnp.float32), 0.1, 1.9)
    pool_weight = gaussian(arg_keys[2], (GROUPS, GROUP_CH, GROUP_CH), GROUP_CH ** -0.5, 0.25, ((0, 4),))
    pool_scale = jnp.clip(1.0 + 0.18 * jax.random.normal(arg_keys[3], (D,), jnp.float32), 0.1, 1.9)
    query_weight = draw_query_weight(jax.random.fold_in(arg_keys[12], 71), part)
    gate_weight = gaussian(arg_keys[5], (D, HEADS), D ** -0.5, 0.125)
    key_weight = gaussian(arg_keys[6], (D, HEADS * HD), D ** -0.5, 0.125, ((1, 4),))
    value_weight = gaussian(arg_keys[7], (D, HEADS * HD), D ** -0.5, 0.125, ((1, 4),))
    out_weight = gaussian(arg_keys[8], (HEADS * HD, D), (HEADS * HD) ** -0.5, 0.1875, ((1, 4),))
    passage_gain = jnp.clip(1.0 + 0.18 * jax.random.normal(arg_keys[9], (D,), jnp.float32), 0.1, 1.9)
    passage_store = gaussian(part_splits[10], (PASSAGES, PLEN, D), 1.0, 6.0, ((0, 32),))
    passage_ids = draw_passage_ids(jax.random.fold_in(jax.random.fold_in(arg_keys[12], part), 71), part)
    return {"tokens": tokens, "norm_gain": norm_gain, "pool_weight": pool_weight, "pool_scale": pool_scale, "query_weight": query_weight, "gate_weight": gate_weight, "key_weight": key_weight, "value_weight": value_weight, "out_weight": out_weight, "passage_gain": passage_gain, "passage_store": passage_store, "passage_ids": passage_ids}


epsilon = 1e-06

def rms_norm(values, gain):
    wide_values = values.astype(jnp.float32)
    inverse = lax.rsqrt(lax.optimization_barrier(jnp.mean(wide_values * wide_values, axis=-1, keepdims=True)) + epsilon)
    return (wide_values * inverse * gain).astype(jnp.bfloat16)

def reference(tokens, norm_gain, pool_weight, pool_scale, query_weight, gate_weight, key_weight, value_weight, out_weight, passage_gain, passage_store, passage_ids):
    normed = rms_norm(tokens, norm_gain)
    sequences = TOKENS // SEQ_LEN
    channels = D // GROUPS
    grouped = normed.astype(jnp.float32).reshape(sequences, SEQ_LEN, GROUPS, channels)
    running = jnp.cumsum(grouped, axis=1)
    position = jnp.arange(SEQ_LEN)
    pieces = []
    for group_index in range(GROUPS):
        window = 2 ** (group_index + 1)
        current = running[:, :, group_index]
        lagged = jnp.pad(current, ((0, 0), (window, 0), (0, 0)))[:, :SEQ_LEN]
        divisor = jnp.minimum(position + 1, window).astype(jnp.float32)[None, :, None]
        pieces.append((current - lagged) / divisor - grouped[:, :, group_index])
    pooled = jnp.stack(pieces, axis=2).astype(jnp.bfloat16).reshape(TOKENS, GROUPS, channels)
    mixing = jnp.einsum('tgc,gcd->tgd', pooled.astype(jnp.float32), pool_weight.astype(jnp.float32)).reshape(TOKENS, D) * pool_scale
    queries = jnp.dot(normed, query_weight, preferred_element_type=jnp.float32).astype(jnp.bfloat16)
    gating = jax.nn.sigmoid(jnp.dot(normed, gate_weight, preferred_element_type=jnp.float32))
    query_blocks = queries.reshape(BLOCKS, BLK, HEADS, HD)
    gate_blocks = gating.reshape(BLOCKS, BLK, HEADS)

    def one_block(inputs):
        block_queries, block_gates, block_ids = inputs
        fetched = jnp.take(passage_store, block_ids, axis=0).reshape(NPB * PLEN, D)
        passage_rows = rms_norm(fetched, passage_gain)
        key_rows = jnp.dot(passage_rows, key_weight, preferred_element_type=jnp.float32).astype(jnp.bfloat16).reshape(NPB * PLEN, HEADS, HD)
        values = jnp.dot(passage_rows, value_weight, preferred_element_type=jnp.float32).astype(jnp.bfloat16).reshape(NPB * PLEN, HEADS, HD)
        scores = jnp.einsum('qhd,khd->hqk', block_queries.astype(jnp.float32), key_rows.astype(jnp.float32)) * HD ** (-0.5)
        row_max = lax.optimization_barrier(jnp.max(scores, axis=-1, keepdims=True))
        weights = jnp.exp(scores - row_max)
        probabilities = (weights / lax.optimization_barrier(jnp.sum(weights, axis=-1, keepdims=True))).astype(jnp.bfloat16)
        attended = jnp.einsum('hqk,khd->qhd', probabilities.astype(jnp.float32), values.astype(jnp.float32))
        return (attended * block_gates[:, :, None]).astype(jnp.bfloat16).reshape(BLK, HEADS * HD)
    head_out = lax.map(one_block, (query_blocks, gate_blocks, passage_ids)).reshape(TOKENS, HEADS * HD)
    crossed = jnp.dot(head_out, out_weight, preferred_element_type=jnp.float32)
    return (mixing + crossed).astype(jnp.bfloat16)
```

```python
import functools

import jax
import jax.numpy as jnp
from jax import lax
from jax.experimental import pallas as pl
from jax.experimental.pallas import tpu as pltpu
from jax.sharding import PartitionSpec as P

HD = 128
GROUPS = 4
SEQ_LEN = 256
BLK = 128
NPB = 4
PLEN = 64
P_DEV = 24
CORES = 2
CHIP_PASSAGES = CORES * P_DEV

LAG = 4
LAND = 16
STAGE = 6
MOST_ROUNDS = 128
LEVELS = (72, 75, 78, 82, 90)

epsilon = 1e-06
MESH = pl.DeviceIdType.MESH


def project_kernel(ids_ref, gain_ref, key_ref, value_ref, store_ref, ring_ref, both_ref,
                   buf, load_sem, id_send, id_recv, kv_send, kv_recv):
    me = lax.axis_index("st")
    count = lax.axis_size("st")
    chips = count // CORES
    core = me % CORES
    chip = me // CORES
    partner = chip * CORES + (1 - core)
    barrier = pltpu.get_barrier_semaphore()
    pl.semaphore_signal(barrier, inc=1, device_id={"st": partner}, device_id_type=MESH)
    for step in range(1, chips):
        peer = lax.rem(chip + step, chips) * CORES + core
        pl.semaphore_signal(barrier, inc=1, device_id={"st": peer}, device_id_type=MESH)
    per = buf.shape[1]
    chunks = P_DEV // per
    rows = per * PLEN

    def load(index):
        return pltpu.make_async_copy(
            store_ref.at[pl.ds(index * per, per)], buf.at[index % 2], load_sem.at[index % 2])

    def give(index):
        there = both_ref.at[core, pl.ds(index * per, per)]
        return pltpu.make_async_remote_copy(
            src_ref=there, dst_ref=there, send_sem=kv_send.at[index], recv_sem=kv_recv.at[index],
            device_id={"st": partner}, device_id_type=MESH)

    def tell(step):
        peer = lax.rem(chip + step, chips) * CORES + core
        return pltpu.make_async_remote_copy(
            src_ref=ids_ref, dst_ref=ring_ref.at[chip],
            send_sem=id_send.at[step], recv_sem=id_recv.at[step],
            device_id={"st": peer}, device_id_type=MESH)

    load(0).start()
    ring_ref[chip] = ids_ref[...]
    for index in range(chunks):
        if index + 1 < chunks:
            load(index + 1).start()
        load(index).wait()
        if index == 1:
            pl.semaphore_wait(barrier, chips)
            for step in range(1, chips):
                tell(step).start()
        wide = buf[index % 2].astype(jnp.float32).reshape(rows, buf.shape[3])
        inverse = lax.rsqrt(jnp.mean(wide * wide, axis=-1, keepdims=True) + epsilon)
        normed = (wide * inverse * gain_ref[...]).astype(jnp.bfloat16)
        width = key_ref.shape[1]
        keys = jnp.dot(normed, key_ref[...], preferred_element_type=jnp.float32)
        values = jnp.dot(normed, value_ref[...], preferred_element_type=jnp.float32)
        own = pl.ds(index * per, per)
        both_ref[core, own, :, :width] = keys.astype(jnp.bfloat16).reshape(per, PLEN, width)
        both_ref[core, own, :, width:] = values.astype(jnp.bfloat16).reshape(per, PLEN, width)
        if index >= 2:
            give(index - 1).start()
        if index == 1:
            give(0).start()
    for step in range(1, chips):
        tell(step).wait()
    give(chunks - 1).start()
    for index in range(chunks):
        give(index).wait()


def project(ids_row, passage_gain, key_weight, value_weight, passage_store, chips):
    width = key_weight.shape[1] + value_weight.shape[1]
    per = 4
    vmem = pl.BlockSpec(memory_space=pltpu.VMEM)
    rows = passage_store.shape[0] * PLEN
    return pl.pallas_call(
        project_kernel,
        name="project_kernel",
        out_shape=(
            jax.ShapeDtypeStruct((chips, 1, ids_row.shape[1]), jnp.int32),
            jax.ShapeDtypeStruct((CORES, P_DEV, PLEN, width), jnp.bfloat16),
        ),
        in_specs=[vmem] * 4 + [pl.BlockSpec(memory_space=pl.ANY)],
        out_specs=(vmem, vmem),
        scratch_shapes=[
            pltpu.VMEM((2, per, PLEN, passage_store.shape[2]), jnp.bfloat16),
            pltpu.SemaphoreType.DMA((2,)),
            pltpu.SemaphoreType.DMA((chips,)),
            pltpu.SemaphoreType.DMA((chips,)),
            pltpu.SemaphoreType.DMA((P_DEV // per,)),
            pltpu.SemaphoreType.DMA((P_DEV // per,)),
        ],
        cost_estimate=pl.CostEstimate(
            flops=2 * rows * passage_store.shape[2] * width,
            bytes_accessed=2 * rows * (passage_store.shape[2] + width),
            transcendentals=0),
        compiler_params=pltpu.CompilerParams(collective_id=0, has_side_effects=True),
    )(ids_row, passage_gain[None, :], key_weight, value_weight, passage_store)


def plan(ring_ids, chip):
    chips = ring_ids.shape[0]
    half = chips // 2
    reads = ring_ids.shape[1]
    source = ring_ids // CHIP_PASSAGES
    passage = ring_ids % CHIP_PASSAGES
    reader = lax.broadcasted_iota(jnp.int32, source.shape, 0)
    order = jnp.arange(reads, dtype=jnp.int32)
    same = (source[:, :, None] == source[:, None, :]) & (order[None, None, :] < order[None, :, None])
    before = jnp.sum(same.astype(jnp.int32), axis=2)
    around = (reader - source + chips) % chips
    turn = (before + reader) % 2
    is_up = ((around >= 1) & (around < half)) | ((around == half) & (turn == 0))
    is_down = (around > half) | ((around == half) & (turn == 1))
    going = jnp.stack([is_up, is_down])
    distance = jnp.stack([around, (chips - around) % chips])
    start = jnp.stack([source, (chips - source) % chips])
    place = jnp.where(around == half, before // 2, before)
    here = jnp.stack([chip, (chips - chip) % chips])
    node = jnp.arange(chips, dtype=jnp.int32)
    hop = jnp.arange(half, dtype=jnp.int32)
    counted = (
        going[:, None, None]
        & (start[:, None, None] == node[None, :, None, None, None])
        & (distance[:, None, None] > hop[None, None, :, None, None])
    )
    further = jnp.sum(counted.astype(jnp.int32), axis=(3, 4))
    starts = [jnp.zeros((2, chips), jnp.int32)]
    for j in range(1, half):
        starts.append(jnp.maximum(
            jnp.roll(starts[-1] + further[:, :, j - 1], -1, axis=1), starts[-1] + LAG))
    begin = jnp.stack(starts, axis=2)
    rounds = jnp.max(jnp.where(further > 0, begin + further, 0))
    upstream = (here[:, None] - hop[None, :] + chips) % chips
    chosen = (node[None, :, None] == upstream[:, None, :]).astype(jnp.int32)
    opens = jnp.sum(chosen * begin, axis=1)
    lengths = jnp.sum(chosen * further, axis=1)
    shifted = jnp.concatenate([jnp.zeros_like(begin[:, :, :1]), begin[:, :, :-1]], axis=2)
    arrived = jnp.sum(chosen * shifted, axis=1)
    clock = jnp.arange(MOST_ROUNDS, dtype=jnp.int32)[None, :, None]
    lane = jnp.arange(2, dtype=jnp.int32)
    active = (
        (clock >= opens[:, None]) & (clock < (opens + lengths)[:, None]) & (hop[None, None] > 0)
    )
    passing = jnp.sum(
        jnp.where(active, CHIP_PASSAGES + lane[:, None, None] + 2 * (arrived[:, None] + clock - opens[:, None]), 0),
        axis=2)
    further_padded = jnp.concatenate([further, jnp.zeros_like(further[:, :, :1])], axis=2)
    steps = jnp.arange(half + 1, dtype=jnp.int32)
    own_further = jnp.sum(
        jnp.where(node[None, :, None] == here[:, None, None], further_padded, 0), axis=1)
    position = place + jnp.sum(
        jnp.where(distance[..., None] == steps, own_further[:, None, None, :], 0), axis=3)
    leaving = going & (source == chip)
    first = jnp.sum(
        jnp.where(leaving[:, None] & (position[:, None] == clock[:, :, :, None]), passage, 0),
        axis=(2, 3))
    sends = passing + first
    row = lax.dynamic_slice_in_dim
    my_going = row(going, chip, 1, axis=1)[:, 0]
    my_start = row(start, chip, 1, axis=1)[:, 0]
    my_distance = row(distance, chip, 1, axis=1)[:, 0]
    my_place = row(place, chip, 1, axis=0)[0]
    my_passage = row(passage, chip, 1, axis=0)[0]
    last = begin + further_padded[:, :, 1:]
    picked = (
        (my_start[:, :, None, None] == node[None, None, :, None])
        & (my_distance[:, :, None, None] == hop[None, None, None, :] + 1)
    )
    arrival = jnp.sum(jnp.where(picked, last[:, None], 0), axis=(2, 3)) + my_place
    lands = jnp.sum(jnp.where(my_going, CHIP_PASSAGES + lane[:, None] + 2 * arrival, 0), axis=0)
    lands = jnp.where(my_going[0] | my_going[1], lands, my_passage)
    table = jnp.concatenate([sends, jnp.pad(lands, (0, MOST_ROUNDS - reads))[None]], axis=0)
    return table, rounds


def ring_kernel(rounds, table_ref, kept_ref, out_ref, pool, land, stage, send_sem, recv_sem):
    me = lax.axis_index("st")
    count = lax.axis_size("st")
    up = lax.rem(me + CORES, count)
    down = lax.rem(me + count - CORES, count)
    target = (up, down)
    barrier = pltpu.get_barrier_semaphore()
    for peer in target:
        pl.semaphore_signal(barrier, inc=1, device_id={"st": peer}, device_id_type=MESH)
    pool[:CHIP_PASSAGES] = kept_ref[...]
    pl.semaphore_wait(barrier, 2)

    def copy(way, index):
        return pltpu.make_async_remote_copy(
            src_ref=stage.at[way, index % STAGE], dst_ref=land.at[way, index % LAND],
            send_sem=send_sem.at[way, index % STAGE], recv_sem=recv_sem.at[way, index % LAND],
            device_id={"st": target[way]}, device_id_type=MESH)

    def put(way, index):
        stage[way, index % STAGE] = pool[table_ref[way, index]]

    def take(way, index):
        pool[CHIP_PASSAGES + 2 * index + way] = land[way, index % LAND]

    def one_round(index, fresh, arriving, sending):
        if arriving:
            for way in range(2):
                copy(way, index - LAG).wait_recv()
        if sending:
            for way in range(2):
                copy(way, index - 1).start()
        if arriving:
            for way in range(2):
                take(way, index - LAG)
        if fresh:
            for way in range(2):
                put(way, index)

    for index in range(LAG):
        one_round(index, True, False, index >= 1)

    def middle(index, carry):
        @pl.when(index >= STAGE)
        def _():
            for way in range(2):
                copy(way, index - STAGE).wait_send()
        one_round(index, True, True, True)
        return carry

    lax.fori_loop(LAG, rounds, middle, 0)
    for index in range(rounds, rounds + LAG):
        one_round(index, False, True, index == rounds)
    for index in range(rounds - STAGE, rounds):
        for way in range(2):
            copy(way, index).wait_send()

    def hand(index, carry):
        out_ref[index] = pool[table_ref[2, index]]
        return carry

    lax.fori_loop(0, out_ref.shape[0], hand, 0)


def ring(rounds, ident, reads, table, kept):
    slot = kept.shape[1:]
    vmem = pl.BlockSpec(memory_space=pltpu.VMEM)
    size = slot[0] * slot[1]
    return pl.pallas_call(
        functools.partial(ring_kernel, rounds),
        name=f"ring_kernel_{rounds}",
        out_shape=jax.ShapeDtypeStruct((reads, *slot), jnp.bfloat16),
        in_specs=[pl.BlockSpec(memory_space=pltpu.SMEM), vmem],
        out_specs=vmem,
        scratch_shapes=[
            pltpu.VMEM((CHIP_PASSAGES + 2 * rounds, *slot), jnp.bfloat16),
            pltpu.VMEM((2, LAND, *slot), jnp.bfloat16),
            pltpu.VMEM((2, STAGE, *slot), jnp.bfloat16),
            pltpu.SemaphoreType.DMA((2, STAGE)),
            pltpu.SemaphoreType.DMA((2, LAND)),
        ],
        cost_estimate=pl.CostEstimate(
            flops=rounds * 10**9, bytes_accessed=rounds * size * 8, transcendentals=0),
        compiler_params=pltpu.CompilerParams(collective_id=ident, has_side_effects=True),
    )(table, kept)


def per_device(
    tokens,
    norm_gain,
    pool_weight,
    pool_scale,
    query_weight,
    gate_weight,
    key_weight,
    value_weight,
    out_weight,
    passage_gain,
    passage_store,
    passage_ids,
):
    head_index = lax.axis_index("tp")
    tok_rows, width_local = tokens.shape
    full_width = width_local * lax.axis_size("tp")
    local_heads = query_weight.shape[1] // HD
    head_width = local_heads * HD
    wide_tokens = tokens.astype(jnp.float32)
    square_sums = lax.psum(jnp.sum(wide_tokens * wide_tokens, axis=1), "tp")
    inverse = lax.rsqrt(square_sums / full_width + epsilon)
    gain_local = lax.dynamic_slice_in_dim(norm_gain, head_index * width_local, width_local)
    normed = (wide_tokens * inverse[:, None] * gain_local[None, :]).astype(jnp.bfloat16)
    sequences = tok_rows // SEQ_LEN
    widest = 2**GROUPS
    window = jnp.left_shift(jnp.int32(2), head_index)
    grouped = normed.astype(jnp.float32).reshape(sequences, SEQ_LEN, width_local)
    running = jnp.cumsum(grouped, axis=1)
    padded = jnp.concatenate(
        [jnp.zeros((sequences, widest, width_local), jnp.float32), running], axis=1
    )
    lagged = lax.dynamic_slice_in_dim(padded, widest - window, SEQ_LEN, axis=1)
    position = jnp.arange(SEQ_LEN, dtype=jnp.int32)
    divisor = jnp.minimum(position + 1, window).astype(jnp.float32)
    pooled = (
        ((running - lagged) / divisor[None, :, None] - grouped)
        .astype(jnp.bfloat16)
        .reshape(tok_rows, width_local)
    )
    mixing = (
        jnp.dot(pooled, pool_weight[0], preferred_element_type=jnp.float32) * pool_scale[None, :]
    )
    gate_columns = lax.dynamic_slice_in_dim(
        gate_weight, head_index * local_heads, local_heads, axis=1
    )
    columns = lax.all_gather(normed, "tp", axis=1, tiled=True)

    flat_ids = passage_ids.reshape(-1)
    reads = flat_ids.shape[0]
    chips = lax.axis_size("st") // CORES
    chip = lax.axis_index("st") // CORES
    ids_row = jnp.pad(flat_ids, (0, 128 - reads))[None, :]
    ring_ids, both = project(ids_row, passage_gain, key_weight, value_weight, passage_store, chips)
    table, rounds = plan(ring_ids[:, 0, :reads], chip)
    kept = both.reshape(CHIP_PASSAGES, PLEN, both.shape[3])
    levels = LEVELS + (MOST_ROUNDS,)
    level = jnp.sum((rounds > jnp.array(LEVELS, jnp.int32)).astype(jnp.int32))
    branches = [
        functools.partial(ring, count, 1 + ident, reads) for ident, count in enumerate(levels)
    ]
    key_values = lax.switch(level, branches, table, kept)

    query_sum = jnp.dot(columns, query_weight, preferred_element_type=jnp.float32)
    gate_sum = jnp.dot(columns, gate_columns, preferred_element_type=jnp.float32)
    queries = query_sum.astype(jnp.bfloat16)
    gating = jax.nn.sigmoid(gate_sum)
    block_count = tok_rows // BLK
    key_values = key_values.reshape(block_count, NPB * PLEN, 2 * head_width)
    key_rows = key_values[:, :, :head_width].reshape(block_count, NPB * PLEN, local_heads, HD)
    values = key_values[:, :, head_width:].reshape(block_count, NPB * PLEN, local_heads, HD)
    query_blocks = queries.reshape(block_count, BLK, local_heads, HD)
    scores = jnp.einsum(
        "bqhd,bkhd->bhqk", query_blocks, key_rows, preferred_element_type=jnp.float32
    ) * HD ** (-0.5)
    row_max = jnp.max(scores, axis=-1, keepdims=True)
    weights = jnp.exp(scores - row_max)
    probabilities = (weights / jnp.sum(weights, axis=-1, keepdims=True)).astype(jnp.bfloat16)
    attended = jnp.einsum(
        "bhqk,bkhd->bqhd", probabilities, values, preferred_element_type=jnp.float32
    ).reshape(tok_rows, local_heads, HD)
    head_out = (attended * gating[:, :, None]).astype(jnp.bfloat16).reshape(tok_rows, head_width)
    crossed = jnp.dot(
        lax.all_gather(head_out, "tp", axis=1, tiled=True),
        out_weight, preferred_element_type=jnp.float32
    )
    return (mixing + crossed).astype(jnp.bfloat16)


def solution(mesh):
    in_specs = (
        P(("grp", "st"), "tp"),
        P(),
        P("tp", None, None),
        P("tp"),
        P(None, "tp"),
        P(),
        P(None, "tp"),
        P(None, "tp"),
        P(None, "tp"),
        P(),
        P(("grp", "st"), None, None),
        P(("grp", "st"), None),
    )
    out_specs = P(("grp", "st"), "tp")
    return jax.shard_map(
        per_device, mesh=mesh, in_specs=in_specs, out_specs=out_specs, check_vma=False
    )
```
